32 devices in a mesh: ep: 32 (over z, y, x, core).
Axes of the slice: x: 2, y: 2, z: 4, core: 2. Of those that a mesh axis runs over, the one named last changes fastest.
Arguments:
- tokens: bfloat16 [384, 2048], P('ep'), may hold values from -6 to 6
- cache_latent: bfloat16 [384, 1024, 512], P('ep'), may hold values from -180 to 180
- cache_rope: bfloat16 [384, 1024, 64], P('ep'), may hold values from -6 to 6
- cache_lengths: int32 [384], P('ep'), may hold values from 1 to 1024, as said below
- expert_ids: int32 [384, 6], P('ep'), may hold values from 0 to 15, as said below
- route_weight: float32 [384, 6], P('ep'), may hold values from 1 to 2
- attn_gain: float32 [2048], replicated, may hold values from 0.1 to 1.9
- q_gain: float32 [512], replicated, may hold values from 0.1 to 1.9
- kv_gain: float32 [512], replicated, may hold values from 0.1 to 1.9
- moe_gain: float32 [2048], replicated, may hold values from 0.1 to 1.9
- w_qdown: bfloat16 [2048, 512], replicated, may hold values from -0.125 to 0.125
- w_kvdown: bfloat16 [2048, 512], replicated, may hold values from -0.125 to 0.125
- w_krope: bfloat16 [2048, 64], replicated, may hold values from -0.125 to 0.125
- w_qup: bfloat16 [512, 1536], replicated, may hold values from -0.25 to 0.25
- w_kup: bfloat16 [512, 1024], replicated, may hold values from -0.5 to 0.5
- w_vup: bfloat16 [512, 1024], replicated, may hold values from -0.25 to 0.25
- w_out: bfloat16 [1024, 2048], replicated, may hold values from -0.1875 to 0.1875
- expert_gate: bfloat16 [32, 2048, 256], P('ep'), may hold values from -0.125 to 0.125
- expert_up: bfloat16 [32, 2048, 256], P('ep'), may hold values from -0.125 to 0.125
- expert_down: bfloat16 [32, 256, 2048], P('ep'), may hold values from -0.25 to 0.25
Outputs:
- mixed: float32 [384, 2048], P('ep')
- new_latent: bfloat16 [384, 512], P('ep')
- new_rope_key: bfloat16 [384, 64], P('ep')
The draws below stay inside these ranges and needn't reach their ends.
Inputs may be any that keep to these rules, and one draw needn't show every extreme that they name: `cache_lengths`: some sequence holds 1024 positions. `expert_ids`: each row names 6 different experts of one group g, numbered g * 16 to g * 16 + 15; among the rows of one device no expert is named more than 5 times, and some expert exactly 5 times.
All inputs are finite; a program needn't handle non-finite values.
Results may differ from the reference program's by a relative error of at most 0.03.
Values may be sent and summed in bfloat16 or wider, within the bound.
A program may use at most 128 MiB of HBM per device.

```python
import jax
import jax.numpy as jnp
from jax import lax

D = 2048
HEADS = 8
Q_RANK = 512
KV_RANK = 512
NOPE_DIM = 128
ROPE_DIM = 64
VALUE_DIM = 128
FF = 512
GROUP_SIZE = 16
TOP_K = 6
SEQ_DEV = 12
CACHE = 1024
TOKENS = 384
EXPERTS = 16
GROUPS = 1
GROUP_MOST = 12
CAPACITY = 5
N_EP = 32


def draw_cache_lengths(key, part):
    block_count = TOKENS // SEQ_DEV
    key_list = jax.random.split(jax.random.fold_in(key, 7), 2)
    factor = jax.random.randint(key_list[0], (block_count, 1), 1, 5)
    upper_bound = CACHE * factor // 4
    raw_bits = jax.random.randint(key_list[1], (block_count, SEQ_DEV), 0, 1 << 30)
    lengths = (1 + raw_bits % upper_bound).reshape(TOKENS)
    lengths = lengths.at[0].set(CACHE)
    return lengths.astype(jnp.int32)


def draw_expert_ids(key, part):
    block_count = TOKENS // SEQ_DEV
    base_key = jax.random.fold_in(key, 13)
    seq_order = jax.vmap(lambda sub_key: jax.random.permutation(sub_key, SEQ_DEV))(jax.random.split(jax.random.fold_in(base_key, 1), block_count))
    group_order = jax.vmap(lambda sub_key: jax.random.permutation(sub_key, GROUPS))(jax.random.split(jax.random.fold_in(base_key, 2), block_count))
    local_table = jax.vmap(lambda sub_key: jax.random.permutation(sub_key, GROUP_SIZE))(jax.random.split(jax.random.fold_in(base_key, 3), block_count * GROUPS)).reshape(block_count, GROUPS, GROUP_SIZE)
    others = max(GROUPS - 1, 1)
    first_run = seq_order < GROUP_MOST
    rest_rank = jnp.maximum(seq_order - GROUP_MOST, 0)
    slot_index = jnp.where(first_run, 0, 1 + rest_rank % others)
    group_rank = jnp.where(first_run, seq_order, rest_rank // others)
    group_ids = jnp.take_along_axis(group_order, slot_index, axis=1)
    spot_index = (group_rank[:, :, None] * TOP_K + jnp.arange(TOP_K, dtype=jnp.int32)[None, None, :]) % GROUP_SIZE
    chosen_tables = local_table[jnp.arange(block_count)[:, None], group_ids]
    local_ids = jnp.take_along_axis(chosen_tables, spot_index, axis=2)
    return (group_ids[:, :, None] * GROUP_SIZE + local_ids).reshape(TOKENS, TOP_K).astype(jnp.int32)


def draw_cache_latent(key, part):
    key_list = jax.random.split(jax.random.fold_in(key, 17), 1)
    values = jnp.clip(jax.random.normal(key_list[0], (TOKENS, CACHE, KV_RANK), jnp.float32), -6.0, 6.0)
    return values.astype(jnp.bfloat16)


def block_levels(key, dims, cuts, least, high):
    loudness = 1.0
    for axis_at, shards_of in cuts:
        steps = jax.random.uniform(jax.random.fold_in(jax.random.fold_in(key, 6), axis_at), (shards_of,), jnp.float32, least / len(cuts), high / len(cuts))
        loudness = loudness * jnp.repeat(jnp.exp(steps), dims[axis_at] // shards_of).reshape((-1,) + (1,) * (len(dims) - 1 - axis_at))
    return loudness


def scatter_about(rng, shape, deviation, limit, cuts=(), held_as=jnp.bfloat16):
    values = jax.random.normal(rng, shape, jnp.float32) * deviation
    if len(cuts) > 0:
        values = block_levels(rng, shape, cuts, -0.22, 0.18) * values
    return jnp.clip(values, min=-limit, max=limit).astype(held_as)


def setup_inputs(seed: int = 0) -> dict:
    arg_keys = jax.random.split(jax.random.key(seed), 21)
    return {
        "tokens": scatter_about(arg_keys[0], (TOKENS, D), 1.0, 6.0, ((0, 32),)),
        "cache_latent": draw_cache_latent(jax.random.fold_in(arg_keys[20], 71), 0),
        "cache_rope": scatter_about(arg_keys[2], (TOKENS, CACHE, ROPE_DIM), 1.0, 6.0, ((0, 32),)),
        "cache_lengths": draw_cache_lengths(jax.random.fold_in(arg_keys[20], 71), 0),
        "expert_ids": draw_expert_ids(jax.random.fold_in(arg_keys[20], 71), 0),
        "route_weight": jnp.clip(1.0 + 1.0 * jax.random.uniform(arg_keys[5], (TOKENS, TOP_K), jnp.float32) ** block_levels(arg_keys[5], (TOKENS, TOP_K), ((0, 32),), -0.2, 0.2), 1.0, 2.0),
        "attn_gain": jnp.clip(1.0 + 0.18 * jax.random.normal(arg_keys[6], (D,), jnp.float32), 0.1, 1.9),
        "q_gain": jnp.clip(1.0 + 0.18 * jax.random.normal(arg_keys[7], (Q_RANK,), jnp.float32), 0.1, 1.9),
        "kv_gain": jnp.clip(1.0 + 0.18 * jax.random.normal(arg_keys[8], (KV_RANK,), jnp.float32), 0.1, 1.9),
        "moe_gain": jnp.clip(1.0 + 0.18 * jax.random.normal(arg_keys[9], (D,), jnp.float32), 0.1, 1.9),
        "w_qdown": scatter_about(arg_keys[10], (D, Q_RANK), D ** -0.5, 0.125),
        "w_kvdown": scatter_about(arg_keys[11], (D, KV_RANK), D ** -0.5, 0.125),
        "w_krope": scatter_about(arg_keys[12], (D, ROPE_DIM), D ** -0.5, 0.125),
        "w_qup": scatter_about(arg_keys[13], (Q_RANK, HEADS * (NOPE_DIM + ROPE_DIM)), Q_RANK ** -0.5, 0.25),
        "w_kup": scatter_about(arg_keys[14], (KV_RANK, HEADS * NOPE_DIM), NOPE_DIM ** -0.5, 0.5),
        "w_vup": scatter_about(arg_keys[15], (KV_RANK, HEADS * VALUE_DIM), KV_RANK ** -0.5, 0.25),
        "w_out": scatter_about(arg_keys[16], (HEADS * VALUE_DIM, D), (HEADS * VALUE_DIM) ** -0.5, 0.1875),
        "expert_gate": scatter_about(arg_keys[17], (EXPERTS * 2, D, FF // 2), D ** -0.5, 0.125, ((0, 32),)),
        "expert_up": scatter_about(arg_keys[18], (EXPERTS * 2, D, FF // 2), D ** -0.5, 0.125, ((0, 32),)),
        "expert_down": scatter_about(arg_keys[19], (EXPERTS * 2, FF // 2, D), FF ** -0.5, 0.25, ((0, 32),)),
    }


EPS = 1e-06
THETA = 10000.0

def norm_gain(values, gain_vec):
    values = values.astype(jnp.float32)
    return values * lax.rsqrt(lax.optimization_barrier(jnp.mean(values * values, axis=-1, keepdims=True)) + EPS) * gain_vec.astype(jnp.float32)

def rotary_angles(lengths):
    half_width = ROPE_DIM // 2
    inverse = THETA ** (-jnp.arange(half_width, dtype=jnp.float32) / half_width)
    return lengths.astype(jnp.float32)[:, None] * inverse[None, :]

def rotate(values, angles):
    half_width = values.shape[-1] // 2
    first_half = values[..., :half_width]
    second = values[..., half_width:]
    cosine = jnp.cos(angles)
    sine_part = jnp.sin(angles)
    return jnp.concatenate([first_half * cosine - second * sine_part, second * cosine + first_half * sine_part], axis=-1)

def routed(moe_in, expert_ids, route_weight, expert_gate, expert_up, expert_down):
    row_count = moe_in.shape[0]
    most_rows = N_EP * CAPACITY
    padded = jnp.concatenate([moe_in, jnp.zeros((1, D), moe_in.dtype)], axis=0)

    def one_half(running, inputs):
        half_index, gate_half, up_half, down_half = inputs
        expert = half_index // 2
        match_mask = expert_ids == expert
        weight_sum = lax.optimization_barrier(jnp.sum(jnp.where(match_mask, route_weight, jnp.zeros_like(route_weight)), axis=1))
        chosen = jnp.nonzero(jnp.any(match_mask, axis=1), size=most_rows, fill_value=row_count)[0].astype(jnp.int32)
        slot_rows = padded[chosen]
        hidden = (jax.nn.silu(jnp.dot(slot_rows, gate_half, preferred_element_type=jnp.float32)) * jnp.dot(slot_rows, up_half, preferred_element_type=jnp.float32)).astype(jnp.bfloat16)
        part_out = jnp.dot(hidden, down_half, preferred_element_type=jnp.float32).astype(jnp.bfloat16).astype(jnp.float32)
        weight_pad = jnp.concatenate([weight_sum, jnp.zeros((1,), weight_sum.dtype)])[chosen]
        running = running.at[chosen].add(weight_pad[:, None] * part_out, mode='drop')
        return (running, None)
    halves = jnp.arange(expert_gate.shape[0], dtype=jnp.int32)
    running, _ = lax.scan(one_half, jnp.zeros((row_count, D), jnp.float32), (halves, expert_gate, expert_up, expert_down))
    return running

def reference(tokens, cache_latent, cache_rope, cache_lengths, expert_ids, route_weight, attn_gain, q_gain, kv_gain, moe_gain, w_qdown, w_kvdown, w_krope, w_qup, w_kup, w_vup, w_out, expert_gate, expert_up, expert_down):
    row_count = tokens.shape[0]
    score_scale = (NOPE_DIM + ROPE_DIM) ** (-0.5)
    normed = norm_gain(tokens, attn_gain).astype(jnp.bfloat16)
    q_low = norm_gain(jnp.dot(normed, w_qdown, preferred_element_type=jnp.float32), q_gain).astype(jnp.bfloat16)
    query_all = jnp.dot(q_low, w_qup, preferred_element_type=jnp.float32).reshape(row_count, HEADS, NOPE_DIM + ROPE_DIM)
    angles = rotary_angles(cache_lengths)
    q_nope = query_all[:, :, :NOPE_DIM].astype(jnp.bfloat16)
    q_rope = rotate(query_all[:, :, NOPE_DIM:], angles[:, None, :]).astype(jnp.bfloat16)
    new_latent = norm_gain(jnp.dot(normed, w_kvdown, preferred_element_type=jnp.float32), kv_gain).astype(jnp.bfloat16)
    new_rope_key = rotate(jnp.dot(normed, w_krope, preferred_element_type=jnp.float32), angles).astype(jnp.bfloat16)
    key_up = w_kup.reshape(KV_RANK, HEADS, NOPE_DIM).astype(jnp.float32)
    q_latent = jnp.einsum('thn,chn->thc', q_nope.astype(jnp.float32), key_up).astype(jnp.bfloat16)
    positions = jnp.arange(CACHE, dtype=jnp.int32)

    def one_sequence(inputs):
        q_lat, q_rot, cached, cached_rope, length, latent, rope_key = inputs
        past = (jnp.dot(q_lat, cached.T, preferred_element_type=jnp.float32) + jnp.dot(q_rot, cached_rope.T, preferred_element_type=jnp.float32)) * score_scale
        past = jnp.where(positions[None, :] < length, past, -jnp.inf)
        own_score = (jnp.dot(q_lat, latent, preferred_element_type=jnp.float32) + jnp.dot(q_rot, rope_key, preferred_element_type=jnp.float32)) * score_scale
        scores = jnp.concatenate([past, own_score[:, None]], axis=1)
        peak = lax.optimization_barrier(jnp.max(scores, axis=1, keepdims=True))
        raw_probs = jnp.exp(scores - peak)
        denom = lax.optimization_barrier(jnp.sum(raw_probs, axis=1, keepdims=True))
        probs = raw_probs.astype(jnp.bfloat16)
        summed = jnp.dot(probs[:, :CACHE], cached, preferred_element_type=jnp.float32) + probs[:, CACHE:].astype(jnp.float32) * latent.astype(jnp.float32)[None, :]
        return (summed / denom).astype(jnp.bfloat16)
    o_latent = lax.map(one_sequence, (q_latent, q_rope, cache_latent, cache_rope, cache_lengths, new_latent, new_rope_key))
    value_up = w_vup.reshape(KV_RANK, HEADS, VALUE_DIM).astype(jnp.float32)
    heads_out = jnp.einsum('thc,chv->thv', o_latent.astype(jnp.float32), value_up).astype(jnp.bfloat16)
    heads_out = heads_out.reshape(row_count, HEADS * VALUE_DIM)
    mixed_attn = (tokens.astype(jnp.float32) + jnp.dot(heads_out, w_out, preferred_element_type=jnp.float32)).astype(jnp.bfloat16)
    moe_in = norm_gain(mixed_attn, moe_gain).astype(jnp.bfloat16)
    moe_out = routed(moe_in, expert_ids, route_weight, expert_gate, expert_up, expert_down)
    mixed = mixed_attn.astype(jnp.float32) + moe_out
    return (mixed, new_latent, new_rope_key)
```

```python
import jax
import jax.numpy as jnp
from jax import lax
from jax.experimental import pallas as pl
from jax.experimental.pallas import tpu as pltpu
from jax.sharding import PartitionSpec as P

HEADS = 8
KV_RANK = 512
NOPE_DIM = 128
ROPE_DIM = 64
VALUE_DIM = 128
GROUP_SIZE = 16
TOP_K = 6
BLOCK_POS = 512
SEQ_DEV = 12


EPS = 1e-06
THETA = 10000.0


def partner(value, axis, bit):
    mask = 2**bit
    pairs = [(source, source ^ mask) for source in range(lax.axis_size(axis))]
    return lax.ppermute(value, axis, pairs)


def norm_gain(values, gain_vec):
    values = values.astype(jnp.float32)
    return values * lax.rsqrt(jnp.mean(values * values, axis=-1, keepdims=True) + EPS) * gain_vec


def rotary_angles(lengths):
    half_width = ROPE_DIM // 2
    inverse = THETA ** (-jnp.arange(half_width, dtype=jnp.float32) / half_width)
    return lengths.astype(jnp.float32)[:, None] * inverse[None, :]


def rotate(values, angles):
    half_width = values.shape[-1] // 2
    first_half = values[..., :half_width]
    second = values[..., half_width:]
    cosine = jnp.cos(angles)
    sine_part = jnp.sin(angles)
    return jnp.concatenate(
        [first_half * cosine - second * sine_part, second * cosine + first_half * sine_part],
        axis=-1,
    )


def attend(
    tokens,
    cache_latent,
    cache_rope,
    cache_lengths,
    attn_gain,
    q_gain,
    kv_gain,
    w_qdown,
    w_kvdown,
    w_krope,
    w_qup,
    w_kup,
    w_vup,
    w_out,
):
    row_count = tokens.shape[0]
    score_scale = (NOPE_DIM + ROPE_DIM) ** (-0.5)
    normed = norm_gain(tokens, attn_gain).astype(jnp.bfloat16)
    q_low = norm_gain(jnp.dot(normed, w_qdown, preferred_element_type=jnp.float32), q_gain).astype(
        jnp.bfloat16
    )
    query_all = jnp.dot(q_low, w_qup, preferred_element_type=jnp.float32).reshape(
        row_count, HEADS, NOPE_DIM + ROPE_DIM
    )
    angles = rotary_angles(cache_lengths)
    q_nope = query_all[:, :, :NOPE_DIM].astype(jnp.bfloat16)
    q_rope = rotate(query_all[:, :, NOPE_DIM:], angles[:, None, :]).astype(jnp.bfloat16)
    new_latent = norm_gain(
        jnp.dot(normed, w_kvdown, preferred_element_type=jnp.float32), kv_gain
    ).astype(jnp.bfloat16)
    new_rope_key = rotate(
        jnp.dot(normed, w_krope, preferred_element_type=jnp.float32), angles
    ).astype(jnp.bfloat16)
    q_latent = jnp.einsum(
        "thn,chn->thc",
        q_nope,
        w_kup.reshape(KV_RANK, HEADS, NOPE_DIM),
        preferred_element_type=jnp.float32,
    ).astype(jnp.bfloat16)
    own_score = (
        jnp.einsum("thc,tc->th", q_latent, new_latent, preferred_element_type=jnp.float32)
        + jnp.einsum("thr,tr->th", q_rope, new_rope_key, preferred_element_type=jnp.float32)
    ) * score_scale
    run_sum = jnp.broadcast_to(
        new_latent.astype(jnp.float32)[:, None, :], (row_count, HEADS, KV_RANK)
    )
    run_total = jnp.ones((row_count, HEADS), jnp.float32)
    block_total = (jnp.max(cache_lengths) + BLOCK_POS - 1) // BLOCK_POS

    def block_step(block_index, carry):
        run_peak, run_total, run_sum = carry
        block_start = block_index * BLOCK_POS
        latent_block = lax.dynamic_slice_in_dim(cache_latent, block_start, BLOCK_POS, 1)
        rope_block = lax.dynamic_slice_in_dim(cache_rope, block_start, BLOCK_POS, 1)
        scores = (
            jnp.einsum("thc,tpc->thp", q_latent, latent_block, preferred_element_type=jnp.float32)
            + jnp.einsum("thr,tpr->thp", q_rope, rope_block, preferred_element_type=jnp.float32)
        ) * score_scale
        valid_mask = (block_start + jnp.arange(BLOCK_POS, dtype=jnp.int32))[
            None, None, :
        ] < cache_lengths[:, None, None]
        scores = jnp.where(valid_mask, scores, -jnp.inf)
        new_peak = jnp.maximum(run_peak, jnp.max(scores, axis=2))
        shrink = jnp.exp(run_peak - new_peak)
        block_probs = jnp.exp(scores - new_peak[:, :, None])
        run_total = run_total * shrink + jnp.sum(block_probs, axis=2)
        run_sum = run_sum * shrink[:, :, None] + jnp.einsum(
            "thp,tpc->thc",
            block_probs.astype(jnp.bfloat16),
            latent_block,
            preferred_element_type=jnp.float32,
        )
        return (new_peak, run_total, run_sum)

    run_peak, run_total, run_sum = lax.fori_loop(
        0, block_total, block_step, (own_score, run_total, run_sum)
    )
    o_latent = (run_sum / run_total[:, :, None]).astype(jnp.bfloat16)
    heads_out = (
        jnp.einsum(
            "thc,chv->thv",
            o_latent,
            w_vup.reshape(KV_RANK, HEADS, VALUE_DIM),
            preferred_element_type=jnp.float32,
        )
        .astype(jnp.bfloat16)
        .reshape(row_count, HEADS * VALUE_DIM)
    )
    mixed_attn = (
        tokens.astype(jnp.float32) + jnp.dot(heads_out, w_out, preferred_element_type=jnp.float32)
    ).astype(jnp.bfloat16)
    return (mixed_attn, new_latent, new_rope_key)


MESH = pl.DeviceIdType.MESH
SUBLANES = 8
LANES = 128


def capacity_of(half_count):
    group_count = half_count // 2 // GROUP_SIZE
    group_most = min(SEQ_DEV, max(3, 2 * ((SEQ_DEV + group_count - 1) // group_count)))
    return (TOP_K * group_most + GROUP_SIZE - 1) // GROUP_SIZE


def remote(src, dst, send_sem, recv_sem, device):
    return pltpu.make_async_remote_copy(
        src_ref=src,
        dst_ref=dst,
        send_sem=send_sem,
        recv_sem=recv_sem,
        device_id=(device,),
        device_id_type=MESH,
    )


def greet_all(me, count):
    barrier = pltpu.get_barrier_semaphore()

    @pl.loop(1, count)
    def _(step):
        pl.semaphore_signal(
            barrier, inc=1, device_id=(lax.rem(me + step, count),), device_id_type=MESH
        )

    pl.semaphore_wait(barrier, count - 1)


def distance(step, count):
    return lax.rem(count // 2 + step + jnp.where(step >= count // 2, 1, 0), count)


def dispatch_kernel(count, out_rows, got, send_sem, recv_sem, pair_send, pair_recv, own_sem):
    me = lax.axis_index("ep")
    core = lax.rem(me, 2)
    sibling = me + 1 - 2 * core
    own = pltpu.make_async_copy(out_rows.at[me], got.at[core, me], own_sem)
    own.start()
    greet_all(me, count)

    @pl.loop(0, count - 1)
    def _(step):
        target = lax.rem(me + distance(step, count), count)
        remote(
            out_rows.at[target],
            got.at[lax.rem(target, 2), me],
            send_sem.at[target],
            recv_sem.at[me],
            target,
        ).start()

    own.wait()
    remote(
        got.at[core, me], got.at[core, me], pair_send.at[me], pair_recv.at[me], sibling
    ).start()

    @pl.loop(0, count - 1)
    def _(step):
        source = lax.rem(me + count - distance(step, count), count)
        place = got.at[core, source]
        remote(
            out_rows.at[source], place, send_sem.at[source], recv_sem.at[source], source
        ).wait_recv()
        remote(place, place, pair_send.at[source], pair_recv.at[source], sibling).start()

    @pl.loop(0, count - 1)
    def _(step):
        target = lax.rem(me + distance(step, count), count)
        remote(
            out_rows.at[target],
            got.at[core, target],
            send_sem.at[target],
            recv_sem.at[target],
            target,
        ).wait_send()

    @pl.loop(0, count)
    def _(source):
        remote(
            got.at[core, source],
            got.at[1 - core, source],
            pair_send.at[source],
            pair_recv.at[source],
            sibling,
        ).wait()


def combine_kernel(
    count, batch, parts, got, from_pair, sums, send_sem, recv_sem, pair_send, pair_recv, own_sem
):
    me = lax.axis_index("ep")
    core = lax.rem(me, 2)
    sibling = me + 1 - 2 * core
    batches = count // batch
    first = me // batch + batches // 2
    greet_all(me, count)

    def pair_copy(index):
        span = pl.ds(index * batch, batch)
        return remote(
            parts.at[1 - core, span],
            from_pair.at[span],
            pair_send.at[index],
            pair_recv.at[index],
            sibling,
        )

    @pl.loop(0, batches)
    def _(step):
        pair_copy(lax.rem(first + step, batches)).start()

    @pl.loop(0, batches)
    def _(step):
        index = lax.rem(first + step, batches)
        pair_copy(index).wait_recv()
        span = pl.ds(index * batch, batch)
        sums[span] = (
            parts[core, span].astype(jnp.float32) + from_pair[span].astype(jnp.float32)
        ).astype(sums.dtype)
        for place in range(batch):
            target = index * batch + place

            @pl.when(target != me)
            def _():
                remote(
                    sums.at[target], got.at[me], send_sem.at[target], recv_sem.at[me], target
                ).start()

    own = pltpu.make_async_copy(sums.at[me], got.at[me], own_sem)
    own.start()

    @pl.loop(0, batches)
    def _(index):
        pair_copy(index).wait_send()

    @pl.loop(1, count)
    def _(step):
        other = lax.rem(me + step, count)
        remote(
            sums.at[other], got.at[other], send_sem.at[other], recv_sem.at[other], other
        ).wait()

    own.wait()


def dispatch(out_rows):
    count = out_rows.shape[0]
    return pl.pallas_call(
        lambda *refs: dispatch_kernel(count, *refs),
        out_shape=jax.ShapeDtypeStruct((2,) + out_rows.shape, out_rows.dtype),
        in_specs=[pl.BlockSpec(memory_space=pltpu.VMEM)],
        out_specs=pl.BlockSpec(memory_space=pltpu.VMEM),
        scratch_shapes=[pltpu.SemaphoreType.DMA((count,))] * 4 + [pltpu.SemaphoreType.DMA],
        compiler_params=pltpu.CompilerParams(collective_id=0, has_side_effects=True),
        name="dispatch",
    )(out_rows)


def combine(parts):
    count = parts.shape[1]
    batch = 4
    return pl.pallas_call(
        lambda *refs: combine_kernel(count, batch, *refs),
        out_shape=jax.ShapeDtypeStruct(parts.shape[1:], parts.dtype),
        in_specs=[pl.BlockSpec(memory_space=pltpu.VMEM)],
        out_specs=pl.BlockSpec(memory_space=pltpu.VMEM),
        scratch_shapes=[pltpu.VMEM(parts.shape[1:], parts.dtype)] * 2
        + [pltpu.SemaphoreType.DMA((count,))] * 2
        + [pltpu.SemaphoreType.DMA((count // batch,))] * 2
        + [pltpu.SemaphoreType.DMA],
        compiler_params=pltpu.CompilerParams(collective_id=1, has_side_effects=True),
        name="combine",
    )(parts)


def route_plan(expert_ids, route_weight, half_count):
    row_count, top_count = expert_ids.shape
    expert_count = half_count // 2
    slot_count = capacity_of(half_count)
    flat_ids = expert_ids.reshape(-1)
    one_hot = (flat_ids[:, None] == jnp.arange(expert_count, dtype=jnp.int32)[None, :]).astype(
        jnp.int32
    )
    earlier = jnp.cumsum(one_hot, axis=0) - one_hot
    slot_rank = jnp.sum(earlier * one_hot, axis=1)
    slot_ids = flat_ids * slot_count + slot_rank
    placed = slot_ids.reshape(row_count, top_count)[:, :, None] == jnp.arange(
        expert_count * slot_count, dtype=jnp.int32
    )
    chosen = jnp.any(placed, axis=1).astype(jnp.bfloat16)
    weights = jnp.sum(jnp.where(placed, route_weight[:, :, None], 0.0), axis=1)
    return chosen, weights


def mix_experts(moe_in, plan, expert_gate, expert_up, expert_down):
    model_width = moe_in.shape[1]
    half_count = lax.axis_size("ep")
    expert_count = half_count // 2
    slot_count = capacity_of(half_count)
    chosen, weights = plan
    pieces = model_width // (2 * SUBLANES * LANES) * SUBLANES
    outgoing = jnp.einsum("sx,sd->xd", chosen, moe_in, preferred_element_type=jnp.float32).astype(
        jnp.bfloat16
    )
    outgoing = (
        outgoing.reshape(expert_count, slot_count, 2, pieces, LANES)
        .transpose(0, 2, 1, 3, 4)
        .reshape(half_count, slot_count, pieces, LANES)
    )
    halves = dispatch(outgoing)
    flat_rows = halves.transpose(1, 2, 0, 3, 4).reshape(half_count * slot_count, model_width)
    hidden = (
        jax.nn.silu(jnp.dot(flat_rows, expert_gate[0], preferred_element_type=jnp.float32))
        * jnp.dot(flat_rows, expert_up[0], preferred_element_type=jnp.float32)
    ).astype(jnp.bfloat16)
    parts = (
        jnp.dot(hidden, expert_down[0], preferred_element_type=jnp.float32)
        .astype(jnp.bfloat16)
        .reshape(half_count, slot_count, 2, pieces, LANES)
        .transpose(2, 0, 1, 3, 4)
    )
    returned = combine(parts)
    returned = (
        returned.reshape(expert_count, 2, slot_count, pieces, LANES)
        .transpose(0, 2, 1, 3, 4)
        .reshape(expert_count * slot_count, model_width)
    )
    return jnp.dot(
        weights,
        returned.astype(jnp.float32),
        precision=lax.Precision.HIGHEST,
        preferred_element_type=jnp.float32,
    )


def shards(
    tokens,
    cache_latent,
    cache_rope,
    cache_lengths,
    expert_ids,
    route_weight,
    attn_gain,
    q_gain,
    kv_gain,
    moe_gain,
    w_qdown,
    w_kvdown,
    w_krope,
    w_qup,
    w_kup,
    w_vup,
    w_out,
    expert_gate,
    expert_up,
    expert_down,
):
    mixer_weights = (
        attn_gain,
        q_gain,
        kv_gain,
        w_qdown,
        w_kvdown,
        w_krope,
        w_qup,
        w_kup,
        w_vup,
        w_out,
    )
    mixed_attn, new_latent, new_rope_key = attend(
        tokens, cache_latent, cache_rope, cache_lengths, *mixer_weights
    )
    moe_in = norm_gain(mixed_attn, moe_gain).astype(jnp.bfloat16)
    plan = route_plan(expert_ids, route_weight, lax.axis_size("ep"))
    moe_out = mix_experts(moe_in, plan, expert_gate, expert_up, expert_down)
    mixed = mixed_attn.astype(jnp.float32) + moe_out
    return (mixed, new_latent, new_rope_key)


def solution(mesh):
    placed = (
        P("ep", None),
        P("ep", None, None),
        P("ep", None, None),
        P("ep"),
        P("ep", None),
        P("ep", None),
        P(),
        P(),
        P(),
        P(),
        P(),
        P(),
        P(),
        P(),
        P(),
        P(),
        P(),
        P("ep", None, None),
        P("ep", None, None),
        P("ep", None, None),
    )
    return jax.shard_map(
        shards,
        mesh=mesh,
        in_specs=placed,
        out_specs=(P("ep", None), P("ep", None), P("ep", None)),
        check_vma=False,
    )
```

```python
import jax
import jax.numpy as jnp
from jax import lax
from jax.experimental import pallas as pl
from jax.experimental.pallas import tpu as pltpu
from jax.sharding import PartitionSpec as P

HEADS = 8
KV_RANK = 512
NOPE_DIM = 128
ROPE_DIM = 64
VALUE_DIM = 128
GROUP_SIZE = 16
TOP_K = 6
BLOCK_POS = 512
FETCH_POS = 256
SEQ_DEV = 12


EPS = 1e-06
THETA = 10000.0


def partner(value, axis, bit):
    mask = 2**bit
    pairs = [(source, source ^ mask) for source in range(lax.axis_size(axis))]
    return lax.ppermute(value, axis, pairs)


def norm_gain(values, gain_vec):
    values = values.astype(jnp.float32)
    return values * lax.rsqrt(jnp.mean(values * values, axis=-1, keepdims=True) + EPS) * gain_vec


def rotary_angles(lengths):
    half_width = ROPE_DIM // 2
    inverse = THETA ** (-jnp.arange(half_width, dtype=jnp.float32) / half_width)
    return lengths.astype(jnp.float32)[:, None] * inverse[None, :]


def rotate(values, angles):
    half_width = values.shape[-1] // 2
    first_half = values[..., :half_width]
    second = values[..., half_width:]
    cosine = jnp.cos(angles)
    sine_part = jnp.sin(angles)
    return jnp.concatenate(
        [first_half * cosine - second * sine_part, second * cosine + first_half * sine_part],
        axis=-1,
    )


def attend_kernel(
    scale, lengths, q_latent, q_rope, own, fresh, latent_hbm, rope_hbm, out,
    latent, rope, scores, probs, sums, latent_sem, rope_sem,
):
    rows, places, _ = latent.shape
    blocks = places // FETCH_POS
    halves = places // BLOCK_POS
    per_half = BLOCK_POS // FETCH_POS

    def copies(row, block):
        span = pl.ds(block * FETCH_POS, FETCH_POS)
        across = (row, slice(None), span)
        return (
            pltpu.make_async_copy(
                latent_hbm.at[row, span], latent.at[row, span], latent_sem.at[row, block]
            ),
            pltpu.make_async_copy(
                rope_hbm.at[across], rope.at[across], rope_sem.at[row, block]
            ),
        )

    @pl.loop(0, rows)
    def _(row):
        for block in range(blocks):
            @pl.when(lengths[row] > block * FETCH_POS)
            def _():
                for copy in copies(row, block):
                    copy.start()

    @pl.loop(0, rows)
    def _(row):
        for block in range(blocks):
            half_start = block // per_half * BLOCK_POS

            @pl.when((lengths[row] <= block * FETCH_POS) & (lengths[row] > half_start))
            def _():
                latent[row, pl.ds(block * FETCH_POS, FETCH_POS)] = jnp.zeros(
                    (FETCH_POS, latent.shape[2]), latent.dtype
                )

    def score(row, half):
        span = pl.ds(half * BLOCK_POS, BLOCK_POS)
        contract = (((1,), (1,)), ((), ()))
        raw = lax.dot_general(
            q_latent[row], latent[row, span], contract, preferred_element_type=jnp.float32
        ) + jnp.dot(
            q_rope[row], rope[row, :, span], preferred_element_type=jnp.float32
        )
        place = half * BLOCK_POS + lax.broadcasted_iota(jnp.int32, raw.shape, 1)
        scores[row, :, span] = jnp.where(place < lengths[row], raw * scale, -jnp.inf)

    for row in range(rows):
        for block in range(blocks):
            @pl.when(lengths[row] > block * FETCH_POS)
            def _():
                for copy in copies(row, block):
                    copy.wait()

        score(row, 0)
        for half in range(1, halves):
            @pl.when(lengths[row] > half * BLOCK_POS)
            def _():
                score(row, half)

            @pl.when(lengths[row] <= half * BLOCK_POS)
            def _():
                scores[row, :, pl.ds(half * BLOCK_POS, BLOCK_POS)] = jnp.full(
                    (scores.shape[1], BLOCK_POS), -jnp.inf, jnp.float32
                )

    values = scores[...]
    own_score = own[...]
    peak = jnp.maximum(jnp.max(values, axis=2, keepdims=True), own_score)
    raised = jnp.exp(values - peak)
    own_prob = jnp.exp(own_score - peak)
    total = jnp.sum(raised, axis=2, keepdims=True) + own_prob
    probs[...] = raised.astype(probs.dtype)
    for row in range(rows):
        sums[row] = jnp.dot(
            probs[row, :, :BLOCK_POS], latent[row, :BLOCK_POS], preferred_element_type=jnp.float32
        )
    for row in range(rows):
        for half in range(1, halves):
            span = pl.ds(half * BLOCK_POS, BLOCK_POS)

            @pl.when(lengths[row] > half * BLOCK_POS)
            def _():
                sums[row] += jnp.dot(
                    probs[row, :, span], latent[row, span], preferred_element_type=jnp.float32
                )

    out[...] = ((sums[...] + own_prob * fresh[...]) / total).astype(out.dtype)


def attend_cached(q_latent, q_rope, own, fresh, lengths, cache_latent, cache_rope, scale):
    rows, places, width = cache_latent.shape
    heads = q_latent.shape[1]
    blocks = places // FETCH_POS
    vmem = pl.BlockSpec(memory_space=pltpu.VMEM)
    hbm = pl.BlockSpec(memory_space=pltpu.HBM)
    read = rows * places * (width + ROPE_DIM)
    return pl.pallas_call(
        lambda *refs: attend_kernel(scale, *refs),
        out_shape=jax.ShapeDtypeStruct((rows, heads, width), jnp.bfloat16),
        in_specs=[pl.BlockSpec(memory_space=pltpu.SMEM)] + [vmem] * 4 + [hbm] * 2,
        out_specs=vmem,
        scratch_shapes=[
            pltpu.VMEM((rows, places, width), cache_latent.dtype),
            pltpu.VMEM((rows, ROPE_DIM, places), cache_rope.dtype),
            pltpu.VMEM((rows, heads, places), jnp.float32),
            pltpu.VMEM((rows, heads, places), jnp.bfloat16),
            pltpu.VMEM((rows, heads, width), jnp.float32),
            pltpu.SemaphoreType.DMA((rows, blocks)),
            pltpu.SemaphoreType.DMA((rows, blocks)),
        ],
        cost_estimate=pl.CostEstimate(
            flops=4 * heads * read, bytes_accessed=2 * read, transcendentals=rows * heads * places
        ),
        name="attend_cached",
    )(lengths, q_latent, q_rope, own, fresh, cache_latent, jnp.swapaxes(cache_rope, 1, 2))


def attend(
    tokens,
    cache_latent,
    cache_rope,
    cache_lengths,
    attn_gain,
    q_gain,
    kv_gain,
    w_qdown,
    w_kvdown,
    w_krope,
    w_qup,
    w_kup,
    w_vup,
    w_out,
):
    row_count = tokens.shape[0]
    score_scale = (NOPE_DIM + ROPE_DIM) ** (-0.5)
    normed = norm_gain(tokens, attn_gain).astype(jnp.bfloat16)
    q_low = norm_gain(jnp.dot(normed, w_qdown, preferred_element_type=jnp.float32), q_gain).astype(
        jnp.bfloat16
    )
    query_all = jnp.dot(q_low, w_qup, preferred_element_type=jnp.float32).reshape(
        row_count, HEADS, NOPE_DIM + ROPE_DIM
    )
    angles = rotary_angles(cache_lengths)
    q_nope = query_all[:, :, :NOPE_DIM].astype(jnp.bfloat16)
    q_rope = rotate(query_all[:, :, NOPE_DIM:], angles[:, None, :]).astype(jnp.bfloat16)
    new_latent = norm_gain(
        jnp.dot(normed, w_kvdown, preferred_element_type=jnp.float32), kv_gain
    ).astype(jnp.bfloat16)
    new_rope_key = rotate(
        jnp.dot(normed, w_krope, preferred_element_type=jnp.float32), angles
    ).astype(jnp.bfloat16)
    q_latent = jnp.einsum(
        "thn,chn->thc",
        q_nope,
        w_kup.reshape(KV_RANK, HEADS, NOPE_DIM),
        preferred_element_type=jnp.float32,
    ).astype(jnp.bfloat16)
    own_score = (
        jnp.einsum("thc,tc->th", q_latent, new_latent, preferred_element_type=jnp.float32)
        + jnp.einsum("thr,tr->th", q_rope, new_rope_key, preferred_element_type=jnp.float32)
    ) * score_scale
    o_latent = attend_cached(
        q_latent,
        q_rope,
        own_score[:, :, None],
        new_latent.astype(jnp.float32)[:, None, :],
        cache_lengths,
        cache_latent,
        cache_rope,
        score_scale,
    )
    heads_out = (
        jnp.einsum(
            "thc,chv->thv",
            o_latent,
            w_vup.reshape(KV_RANK, HEADS, VALUE_DIM),
            preferred_element_type=jnp.float32,
        )
        .astype(jnp.bfloat16)
        .reshape(row_count, HEADS * VALUE_DIM)
    )
    mixed_attn = (
        tokens.astype(jnp.float32) + jnp.dot(heads_out, w_out, preferred_element_type=jnp.float32)
    ).astype(jnp.bfloat16)
    return (mixed_attn, new_latent, new_rope_key)


MESH = pl.DeviceIdType.MESH
SUBLANES = 8
LANES = 128


def capacity_of(half_count):
    group_count = half_count // 2 // GROUP_SIZE
    group_most = min(SEQ_DEV, max(3, 2 * ((SEQ_DEV + group_count - 1) // group_count)))
    return (TOP_K * group_most + GROUP_SIZE - 1) // GROUP_SIZE


def remote(src, dst, send_sem, recv_sem, device):
    return pltpu.make_async_remote_copy(
        src_ref=src,
        dst_ref=dst,
        send_sem=send_sem,
        recv_sem=recv_sem,
        device_id=(device,),
        device_id_type=MESH,
    )


def greet_all(me, count):
    barrier = pltpu.get_barrier_semaphore()

    @pl.loop(1, count)
    def _(step):
        pl.semaphore_signal(
            barrier, inc=1, device_id=(lax.rem(me + step, count),), device_id_type=MESH
        )

    pl.semaphore_wait(barrier, count - 1)


def distance(step, count):
    return lax.rem(count // 2 + step + jnp.where(step >= count // 2, 1, 0), count)


def dispatch_kernel(count, out_rows, got, send_sem, recv_sem, pair_send, pair_recv, own_sem):
    me = lax.axis_index("ep")
    core = lax.rem(me, 2)
    sibling = me + 1 - 2 * core
    own = pltpu.make_async_copy(out_rows.at[me], got.at[core, me], own_sem)
    own.start()
    greet_all(me, count)

    @pl.loop(0, count - 1)
    def _(step):
        target = lax.rem(me + distance(step, count), count)
        remote(
            out_rows.at[target],
            got.at[lax.rem(target, 2), me],
            send_sem.at[target],
            recv_sem.at[me],
            target,
        ).start()

    own.wait()
    remote(
        got.at[core, me], got.at[core, me], pair_send.at[me], pair_recv.at[me], sibling
    ).start()

    @pl.loop(0, count - 1)
    def _(step):
        source = lax.rem(me + count - distance(step, count), count)
        place = got.at[core, source]
        remote(
            out_rows.at[source], place, send_sem.at[source], recv_sem.at[source], source
        ).wait_recv()
        remote(place, place, pair_send.at[source], pair_recv.at[source], sibling).start()

    @pl.loop(0, count - 1)
    def _(step):
        target = lax.rem(me + distance(step, count), count)
        remote(
            out_rows.at[target],
            got.at[core, target],
            send_sem.at[target],
            recv_sem.at[target],
            target,
        ).wait_send()

    @pl.loop(0, count)
    def _(source):
        remote(
            got.at[core, source],
            got.at[1 - core, source],
            pair_send.at[source],
            pair_recv.at[source],
            sibling,
        ).wait()


def combine_kernel(
    count, batch, parts, got, from_pair, sums, send_sem, recv_sem, pair_send, pair_recv, own_sem
):
    me = lax.axis_index("ep")
    core = lax.rem(me, 2)
    sibling = me + 1 - 2 * core
    batches = count // batch
    first = me // batch + batches // 2
    greet_all(me, count)

    def pair_copy(index):
        span = pl.ds(index * batch, batch)
        return remote(
            parts.at[1 - core, span],
            from_pair.at[span],
            pair_send.at[index],
            pair_recv.at[index],
            sibling,
        )

    @pl.loop(0, batches)
    def _(step):
        pair_copy(lax.rem(first + step, batches)).start()

    @pl.loop(0, batches)
    def _(step):
        index = lax.rem(first + step, batches)
        pair_copy(index).wait_recv()
        span = pl.ds(index * batch, batch)
        sums[span] = (
            parts[core, span].astype(jnp.float32) + from_pair[span].astype(jnp.float32)
        ).astype(sums.dtype)
        for place in range(batch):
            target = index * batch + place

            @pl.when(target != me)
            def _():
                remote(
                    sums.at[target], got.at[me], send_sem.at[target], recv_sem.at[me], target
                ).start()

    own = pltpu.make_async_copy(sums.at[me], got.at[me], own_sem)
    own.start()

    @pl.loop(0, batches)
    def _(index):
        pair_copy(index).wait_send()

    @pl.loop(1, count)
    def _(step):
        other = lax.rem(me + step, count)
        remote(
            sums.at[other], got.at[other], send_sem.at[other], recv_sem.at[other], other
        ).wait()

    own.wait()


def dispatch(out_rows):
    count = out_rows.shape[0]
    return pl.pallas_call(
        lambda *refs: dispatch_kernel(count, *refs),
        out_shape=jax.ShapeDtypeStruct((2,) + out_rows.shape, out_rows.dtype),
        in_specs=[pl.BlockSpec(memory_space=pltpu.VMEM)],
        out_specs=pl.BlockSpec(memory_space=pltpu.VMEM),
        scratch_shapes=[pltpu.SemaphoreType.DMA((count,))] * 4 + [pltpu.SemaphoreType.DMA],
        compiler_params=pltpu.CompilerParams(collective_id=0, has_side_effects=True),
        name="dispatch",
    )(out_rows)


def combine(parts):
    count = parts.shape[1]
    batch = 4
    return pl.pallas_call(
        lambda *refs: combine_kernel(count, batch, *refs),
        out_shape=jax.ShapeDtypeStruct(parts.shape[1:], parts.dtype),
        in_specs=[pl.BlockSpec(memory_space=pltpu.VMEM)],
        out_specs=pl.BlockSpec(memory_space=pltpu.VMEM),
        scratch_shapes=[pltpu.VMEM(parts.shape[1:], parts.dtype)] * 2
        + [pltpu.SemaphoreType.DMA((count,))] * 2
        + [pltpu.SemaphoreType.DMA((count // batch,))] * 2
        + [pltpu.SemaphoreType.DMA],
        compiler_params=pltpu.CompilerParams(collective_id=1, has_side_effects=True),
        name="combine",
    )(parts)


def route_plan(expert_ids, route_weight, half_count):
    row_count, top_count = expert_ids.shape
    expert_count = half_count // 2
    slot_count = capacity_of(half_count)
    flat_ids = expert_ids.reshape(-1)
    one_hot = (flat_ids[:, None] == jnp.arange(expert_count, dtype=jnp.int32)[None, :]).astype(
        jnp.int32
    )
    earlier = jnp.cumsum(one_hot, axis=0) - one_hot
    slot_rank = jnp.sum(earlier * one_hot, axis=1)
    slot_ids = flat_ids * slot_count + slot_rank
    placed = slot_ids.reshape(row_count, top_count)[:, :, None] == jnp.arange(
        expert_count * slot_count, dtype=jnp.int32
    )
    chosen = jnp.any(placed, axis=1).astype(jnp.bfloat16)
    weights = jnp.sum(jnp.where(placed, route_weight[:, :, None], 0.0), axis=1)
    return chosen, weights


def mix_experts(moe_in, plan, expert_gate, expert_up, expert_down):
    model_width = moe_in.shape[1]
    half_count = lax.axis_size("ep")
    expert_count = half_count // 2
    slot_count = capacity_of(half_count)
    chosen, weights = plan
    pieces = model_width // (2 * SUBLANES * LANES) * SUBLANES
    outgoing = jnp.einsum("sx,sd->xd", chosen, moe_in, preferred_element_type=jnp.float32).astype(
        jnp.bfloat16
    )
    outgoing = (
        outgoing.reshape(expert_count, slot_count, 2, pieces, LANES)
        .transpose(0, 2, 1, 3, 4)
        .reshape(half_count, slot_count, pieces, LANES)
    )
    halves = dispatch(outgoing)
    flat_rows = halves.transpose(1, 2, 0, 3, 4).reshape(half_count * slot_count, model_width)
    hidden = (
        jax.nn.silu(jnp.dot(flat_rows, expert_gate[0], preferred_element_type=jnp.float32))
        * jnp.dot(flat_rows, expert_up[0], preferred_element_type=jnp.float32)
    ).astype(jnp.bfloat16)
    parts = (
        jnp.dot(hidden, expert_down[0], preferred_element_type=jnp.float32)
        .astype(jnp.bfloat16)
        .reshape(half_count, slot_count, 2, pieces, LANES)
        .transpose(2, 0, 1, 3, 4)
    )
    returned = combine(parts)
    returned = (
        returned.reshape(expert_count, 2, slot_count, pieces, LANES)
        .transpose(0, 2, 1, 3, 4)
        .reshape(expert_count * slot_count, model_width)
    )
    return jnp.dot(
        weights,
        returned.astype(jnp.float32),
        precision=lax.Precision.HIGHEST,
        preferred_element_type=jnp.float32,
    )


def shards(
    tokens,
    cache_latent,
    cache_rope,
    cache_lengths,
    expert_ids,
    route_weight,
    attn_gain,
    q_gain,
    kv_gain,
    moe_gain,
    w_qdown,
    w_kvdown,
    w_krope,
    w_qup,
    w_kup,
    w_vup,
    w_out,
    expert_gate,
    expert_up,
    expert_down,
):
    mixer_weights = (
        attn_gain,
        q_gain,
        kv_gain,
        w_qdown,
        w_kvdown,
        w_krope,
        w_qup,
        w_kup,
        w_vup,
        w_out,
    )
    mixed_attn, new_latent, new_rope_key = attend(
        tokens, cache_latent, cache_rope, cache_lengths, *mixer_weights
    )
    moe_in = norm_gain(mixed_attn, moe_gain).astype(jnp.bfloat16)
    plan = route_plan(expert_ids, route_weight, lax.axis_size("ep"))
    moe_out = mix_experts(moe_in, plan, expert_gate, expert_up, expert_down)
    mixed = mixed_attn.astype(jnp.float32) + moe_out
    return (mixed, new_latent, new_rope_key)


def solution(mesh):
    placed = (
        P("ep", None),
        P("ep", None, None),
        P("ep", None, None),
        P("ep"),
        P("ep", None),
        P("ep", None),
        P(),
        P(),
        P(),
        P(),
        P(),
        P(),
        P(),
        P(),
        P(),
        P(),
        P(),
        P("ep", None, None),
        P("ep", None, None),
        P("ep", None, None),
    )
    return jax.shard_map(
        shards,
        mesh=mesh,
        in_specs=placed,
        out_specs=(P("ep", None), P("ep", None), P("ep", None)),
        check_vma=False,
    )
```
